32 devices in a mesh: ep: 8 (over z, x), tp: 4 (over y, core).
Axes of the slice: x: 2, y: 2, z: 4, core: 2. Of those that a mesh axis runs over, the one named last changes fastest.
Arguments:
- tokens: bfloat16 [512, 4096], P('ep'), may hold values from -6 to 6
- state_in: float32 [512, 4096], P('ep', 'tp'), may hold values from -6 to 6
- conv_in: bfloat16 [512, 3, 4096], P('ep', None, 'tp'), may hold values from -6 to 6
- mix_gain: bfloat16 [4096], replicated, may hold values from 0.099609375 to 1.8984375
- rnn_weight: bfloat16 [4096, 4096], P('ep', 'tp'), may hold values from -0.09375 to 0.09375
- gate_weight: bfloat16 [4096, 4096], P('ep', 'tp'), may hold values from -0.09375 to 0.09375
- conv_weight: bfloat16 [4, 4096], P(None, 'tp'), may hold values from -3 to 3
- rate_weight: bfloat16 [16, 256, 256], P('tp'), may hold values from -0.375 to 0.375
- input_weight: bfloat16 [16, 256, 256], P('tp'), may hold values from -0.375 to 0.375
- rate_param: float32 [4096], P('tp'), may hold values from 1 to 6
- out_weight: bfloat16 [4096, 4096], P('tp'), may hold values from -0.09375 to 0.09375
- moe_gain: bfloat16 [4096], replicated, may hold values from 0.099609375 to 1.8984375
- expert_gate: bfloat16 [8, 4096, 2048], P('ep', None, 'tp'), may hold values from -0.09375 to 0.09375
- expert_up: bfloat16 [8, 4096, 2048], P('ep', None, 'tp'), may hold values from -0.09375 to 0.09375
- expert_down: bfloat16 [8, 2048, 4096], P('ep', 'tp'), may hold values from -0.125 to 0.125
- routes: int32 [512, 2], P('ep'), may hold values from 0 to 7, all different within a row; in each aligned block of 64 rows (0 to 63, 64 to 127, ...) at most 32 rows name the same one
- route_prob: float32 [512, 2], P('ep'), may hold values from 0.1 to 1
Outputs:
- layer_out: bfloat16 [512, 4096], P('ep', 'tp')
- state_out: float32 [512, 4096], P('ep', 'tp')
- conv_out: bfloat16 [512, 3, 4096], P('ep', None, 'tp')
The draws below stay inside these ranges and needn't reach their ends.
Inputs may be any that keep to these rules, and one draw needn't show every extreme that they name: `routes`: the 2 experts of a sequence differ. Among the rows of one index of ep no expert is named more than 32 times, and in every draw some expert is named exactly 32 times there.
All inputs are finite; a program needn't handle non-finite values.
Results may differ from the reference program's by a relative error of at most 0.014.
Values may be sent and summed in bfloat16 or wider, within the bound.
A program may use at most 64 MiB of HBM per device.

```python
import math
import jax
import jax.numpy as jnp
import numpy as np
from jax import lax

D = 4096
D_RNN = 4096
RG_BLOCKS = 16
RG_BW = 256
FF_E = 2048
TOPK = 2
SEQ_GRP = 64
BATCH = 512
EXPERTS = 8
CAP = 32
N_EP = 8
N_TP = 4


def shard_levels(rng, extent, split, low, high):
    def one(dim, shards_of):
        steps = jax.random.uniform(jax.random.fold_in(jax.random.fold_in(rng, 6), dim), (shards_of,), jnp.float32, low / len(split), high / len(split))
        return jnp.repeat(jnp.exp(steps), extent[dim] // shards_of).reshape((-1,) + (1,) * (len(extent) - dim - 1))

    loudness = one(*split[0])
    for cut in split[1:]:
        loudness = loudness * one(*cut)
    return loudness


def assign_block(key, own, number, rows, amount, top, reach, lean):
    ranking = jax.random.permutation(key, amount)
    crowded, ordinary = portions_of(amount, rows * top, reach, lean, True), portions_of(amount, rows * top, reach, lean, False)
    places = jnp.arange(amount)

    def named(tallies, offset_by):
        used = int((tallies > 0).sum())
        fixed = max(1, used // 4)
        passed = fixed + (places - fixed + offset_by * (used - fixed)) % max(1, amount - fixed)
        return jnp.zeros((amount,), jnp.int32).at[ranking[jnp.where(places < fixed, places, passed)]].set(jnp.asarray(tallies, jnp.int32))

    tallies = jnp.where(number % 4 == 0, named(crowded, number // 4), named(ordinary, number - number // 4 - 1))
    mixed = jax.random.permutation(jax.random.fold_in(own, 3), amount)
    source_of, taker = mixed[0:amount // 2 * 2:2], mixed[1:amount // 2 * 2:2]
    room = jnp.minimum(tallies[source_of] - 1, reach - tallies[taker]) // 2
    room = jnp.where((source_of == ranking[0]) | (taker == ranking[0]) | (tallies[taker] == 0), 0, jnp.maximum(room, 0))
    passed = jax.random.randint(jax.random.fold_in(own, 4), (amount // 2,), 0, 1 << 20) % (room + 1)
    tallies = tallies.at[source_of].add(-passed).at[taker].add(passed)
    items = jnp.searchsorted(jnp.cumsum(tallies), jnp.arange(rows * top), side="right").astype(jnp.int32)
    table = items.reshape(top, rows).T
    table = table[jax.random.permutation(jax.random.fold_in(own, 1), rows)]
    offset_by = jax.random.randint(jax.random.fold_in(own, 2), (rows, 1), 0, top)
    return jnp.take_along_axis(table, (jnp.arange(top)[None, :] + offset_by) % top, axis=1)


def portions_of(number_of, total, limit, slope, full):
    portions = [(1 << 20) // math.isqrt(standing ** slope) + 1 for standing in range(1, number_of + 1)]
    largest = limit if full else min(limit, max(-(-total // number_of), total * portions[0] // sum(portions)))
    least = 1 if total - largest >= number_of - 1 else 0
    given, spare = [largest] + [least] * (number_of - 1), total - largest - least * (number_of - 1)
    while spare > 0:
        movable = [i for i in range(1, number_of) if given[i] < largest] or [i for i in range(1, number_of) if given[i] < limit]
        whole, budget = sum([portions[i] for i in movable]), spare
        for i in movable:
            addition = min(limit - given[i], max(1, budget * portions[i] // whole), spare)
            given[i] = given[i] + addition
            spare = spare - addition
    return np.array(given)


def scatter_about(own_key, dims, scale, limit, shards=(), held_as=jnp.bfloat16):
    level = shard_levels(own_key, dims, shards, -0.22, 0.18) if shards else 1.0
    drawn = jax.random.normal(own_key, dims, jnp.float32) * scale * level
    return jnp.minimum(jnp.maximum(drawn, -limit), limit).astype(held_as)


def setup_inputs(seed: int = 0) -> dict:
    streams_of = jax.random.split(jax.random.key(seed), 18)
    tokens = scatter_about(streams_of[0], (BATCH, D), 1.0, 6.0, ((0, 8),))
    state_in = scatter_about(streams_of[1], (BATCH, D_RNN), 1.0, 6.0, ((0, 8), (1, 4)), jnp.float32)
    conv_in = scatter_about(streams_of[2], (BATCH, 3, D_RNN), 1.0, 6.0, ((0, 8), (2, 4)))
    mix_gain = jnp.clip(1.0 + 0.18 * jax.random.normal(streams_of[3], (D,), jnp.float32), 0.099609375, 1.8984375).astype(jnp.bfloat16)
    rnn_weight = scatter_about(streams_of[4], (D, D_RNN), D ** -0.5, 0.09375, ((0, 8), (1, 4)))
    gate_weight = scatter_about(streams_of[5], (D, D_RNN), D ** -0.5, 0.09375, ((0, 8), (1, 4)))
    conv_weight = scatter_about(streams_of[6], (4, D_RNN), 0.5, 3.0, ((1, 4),))
    rate_weight = scatter_about(streams_of[7], (RG_BLOCKS, RG_BW, RG_BW), RG_BW ** -0.5, 0.375, ((0, 4),))
    input_weight = scatter_about(streams_of[8], (RG_BLOCKS, RG_BW, RG_BW), RG_BW ** -0.5, 0.375, ((0, 4),))
    rate_param = jnp.clip(1.0 + 5.0 * jax.random.uniform(streams_of[9], (D_RNN,), jnp.float32) ** shard_levels(streams_of[9], (D_RNN,), ((0, 4),), -0.2, 0.2), 1.0, 6.0)
    out_weight = scatter_about(streams_of[10], (D_RNN, D), D_RNN ** -0.5, 0.09375, ((0, 4),))
    moe_gain = jnp.clip(1.0 + 0.18 * jax.random.normal(streams_of[11], (D,), jnp.float32), 0.099609375, 1.8984375).astype(jnp.bfloat16)
    expert_gate = scatter_about(streams_of[12], (EXPERTS, D, FF_E), D ** -0.5, 0.09375, ((0, 8), (2, 4)))
    expert_up = scatter_about(streams_of[13], (EXPERTS, D, FF_E), D ** -0.5, 0.09375, ((0, 8), (2, 4)))
    expert_down = scatter_about(streams_of[14], (EXPERTS, FF_E, D), FF_E ** -0.5, 0.125, ((0, 8), (1, 4)))
    routes_keys = jax.random.split(jax.random.fold_in(streams_of[15], 1), BATCH // SEQ_GRP)
    routes_turns = jax.random.permutation(jax.random.fold_in(streams_of[15], 3), BATCH // SEQ_GRP)
    routes = jax.vmap(lambda own, number: assign_block(jax.random.fold_in(streams_of[15], 2), own, number, SEQ_GRP, EXPERTS, TOPK, CAP, 2))(routes_keys, routes_turns).reshape((BATCH, TOPK))
    route_prob = jnp.clip(0.1 + 0.9 * jax.random.uniform(streams_of[16], (BATCH, TOPK), jnp.float32) ** shard_levels(streams_of[16], (BATCH, TOPK), ((0, 8),), -0.2, 0.2), 0.1, 1.0)
    return dict(tokens=tokens, state_in=state_in, conv_in=conv_in, mix_gain=mix_gain, rnn_weight=rnn_weight, gate_weight=gate_weight, conv_weight=conv_weight, rate_weight=rate_weight, input_weight=input_weight, rate_param=rate_param, out_weight=out_weight, moe_gain=moe_gain, expert_gate=expert_gate, expert_up=expert_up, expert_down=expert_down, routes=routes, route_prob=route_prob)


def rms_scale(values, gain):
    scale = lax.rsqrt(lax.optimization_barrier(jnp.mean(values * values, axis=-1, keepdims=True)) + 1e-06)
    return values * scale * gain.astype(jnp.float32)

def slot_targets(route_ids, experts, capacity):
    flat_ids = route_ids.reshape(-1)
    onehot = (flat_ids[:, None] == jnp.arange(experts, dtype=jnp.int32)[None, :]).astype(jnp.int32)
    before = jnp.cumsum(onehot, axis=0) - onehot
    slot_ids = lax.optimization_barrier(jnp.sum(before * onehot, axis=1))
    return (flat_ids * capacity + slot_ids).astype(jnp.int32)

def block_map(conv, weight):
    rows = conv.shape[0]
    parts = conv.reshape(rows, RG_BLOCKS, RG_BW).astype(jnp.float32)
    mapped = jnp.einsum('snc,ncd->snd', parts, weight.astype(jnp.float32))
    return mapped.reshape(rows, D_RNN)

def run_expert(args):
    rows, w_gate, w_up, w_down = args
    rows32 = rows.astype(jnp.float32)
    gate_part = jnp.dot(rows32, w_gate.astype(jnp.float32))
    up_part = jnp.dot(rows32, w_up.astype(jnp.float32))
    hidden = (jax.nn.silu(gate_part) * up_part).astype(jnp.bfloat16)
    split_hidden = hidden.reshape(rows.shape[0], N_TP, FF_E // N_TP).astype(jnp.float32)
    split_down = w_down.reshape(N_TP, FF_E // N_TP, D).astype(jnp.float32)
    pieces = jnp.einsum('rtf,tfd->trd', split_hidden, split_down)
    rounded = lax.optimization_barrier(pieces.astype(jnp.bfloat16)).astype(jnp.float32)
    return lax.optimization_barrier(jnp.sum(rounded, axis=0)).astype(jnp.bfloat16)

def reference(tokens, state_in, conv_in, mix_gain, rnn_weight, gate_weight, conv_weight, rate_weight, input_weight, rate_param, out_weight, moe_gain, expert_gate, expert_up, expert_down, routes, route_prob):
    base = tokens.astype(jnp.float32)
    normed = rms_scale(base, mix_gain).astype(jnp.bfloat16)
    proj_x = jnp.dot(normed, rnn_weight, preferred_element_type=jnp.float32)
    proj_y = jnp.dot(normed, gate_weight, preferred_element_type=jnp.float32)
    moved = proj_x.astype(jnp.bfloat16)
    conv_out = jnp.concatenate([conv_in[:, 1:], moved[:, None, :]], axis=1)
    taps = conv_weight.astype(jnp.float32)
    history = conv_in.astype(jnp.float32)
    summed = history[:, 0] * taps[0] + history[:, 1] * taps[1] + history[:, 2] * taps[2] + moved.astype(jnp.float32) * taps[3]
    conv = summed.astype(jnp.bfloat16)
    rate = jax.nn.sigmoid(block_map(conv, rate_weight))
    in_gate = jax.nn.sigmoid(block_map(conv, input_weight))
    log_decay = -8.0 * rate * jax.nn.softplus(-rate_param)
    state_out = jnp.exp(log_decay) * state_in + jnp.sqrt(-jnp.expm1(2.0 * log_decay)) * in_gate * conv.astype(jnp.float32)
    gated = (state_out * jax.nn.gelu(proj_y, approximate=True)).astype(jnp.bfloat16)
    split_gated = gated.reshape(BATCH, N_TP, D_RNN // N_TP).astype(jnp.float32)
    split_out = out_weight.reshape(N_TP, D_RNN // N_TP, D).astype(jnp.float32)
    pieces = jnp.einsum('btc,tcd->tbd', split_gated, split_out)
    rounded = lax.optimization_barrier(pieces.astype(jnp.bfloat16)).astype(jnp.float32)
    mixed = base + lax.optimization_barrier(jnp.sum(rounded, axis=0))
    normed2 = rms_scale(mixed, moe_gain).astype(jnp.bfloat16)
    group_routes = routes.reshape(N_EP, SEQ_GRP * TOPK)
    targets = jax.vmap(lambda group_ids: slot_targets(group_ids, EXPERTS, CAP))(group_routes)
    dispatch = (jnp.arange(EXPERTS * CAP, dtype=jnp.int32)[None, :, None] == targets[:, None, :]).astype(jnp.float32)
    repeated = jnp.repeat(normed2, TOPK, axis=0).reshape(N_EP, SEQ_GRP * TOPK, D).astype(jnp.float32)
    send = jnp.einsum('grj,gjd->grd', dispatch, repeated).astype(jnp.bfloat16)
    by_expert = send.reshape(N_EP, EXPERTS, CAP, D).transpose(1, 0, 2, 3).reshape(EXPERTS, N_EP * CAP, D)
    outputs = lax.map(run_expert, (by_expert, expert_gate, expert_up, expert_down))
    back = outputs.reshape(EXPERTS, N_EP, CAP, D).transpose(1, 0, 2, 3).reshape(N_EP, EXPERTS * CAP, D).astype(jnp.float32)
    picked = jnp.einsum('grj,grd->gjd', dispatch, back).reshape(BATCH, TOPK, D)
    weights = route_prob / lax.optimization_barrier(jnp.sum(route_prob, axis=1, keepdims=True))
    experts_sum = lax.optimization_barrier(jnp.sum(picked * weights[:, :, None], axis=1))
    layer_out = (mixed + experts_sum).astype(jnp.bfloat16)
    return (layer_out, state_out, conv_out)
```

```python
import functools

import jax
import jax.numpy as jnp
from jax import lax
from jax.experimental import pallas as pl
from jax.experimental.pallas import tpu as pltpu
from jax.sharding import PartitionSpec as P

MESH = pl.DeviceIdType.MESH
F32 = jnp.float32
BF16 = jnp.bfloat16


def dot(a, b):
    return jnp.dot(a, b, preferred_element_type=F32)


def remote(src, dst, send, recv, where):
    return pltpu.make_async_remote_copy(
        src_ref=src, dst_ref=dst, send_sem=send, recv_sem=recv, device_id=where, device_id_type=MESH
    )


def kernel(
    n, p, cap,
    tokens, state_in, hist, mix_gain, moe_gain, conv_w, rate_param, routes, prob,
    rnn_h, gate_h, rate_h, input_h, out_h, eg_h, eu_h, ed_h,
    layer_out, state_out, moved_out,
    wr, wg, wrate, winput, wout, weg, weu, wed,
    normed, cols, part, rbuf, gated,
    op_p, op_o, op_r, hs, hr, mixed,
    sd, rows, xn, hid, e_p, e_o, e_r, es, er, outb, ret,
    wsem, sa, ra, sb, rb, sd1, rd1, sd2, rd2, sc1, rc1, sc2, rc2, sc3, rc3,
    se1, re1, se2, re2, se3, re3,
):
    e = lax.axis_index("ep")
    t = lax.axis_index("tp")
    core = lax.rem(t, 2)
    y = t // 2
    q = t + 1 - 2 * core
    ys = p // 2
    rows_g, width = tokens.shape
    depth = width // n
    chans = rnn_h.shape[1]
    share = width // p
    slots = n * cap

    loads = [
        pltpu.make_async_copy(a, b, wsem.at[i])
        for i, (a, b) in enumerate(
            [(rnn_h, wr), (gate_h, wg), (rate_h, wrate), (input_h, winput), (out_h, wout),
             (eg_h.at[0], weg), (eu_h.at[0], weu), (ed_h.at[0], wed)]
        )
    ]
    for load in loads:
        load.start()

    barrier = pltpu.get_barrier_semaphore()

    @pl.loop(1, n)
    def _(d):
        pl.semaphore_signal(barrier, inc=1, device_id={"ep": lax.rem(e + d, n)}, device_id_type=MESH)

    @pl.loop(1, p)
    def _(d):
        pl.semaphore_signal(barrier, inc=1, device_id={"tp": lax.rem(t + d, p)}, device_id_type=MESH)

    ssq = jnp.zeros((rows_g, 1), F32)
    for j in range(n):
        v = tokens[:, j * depth:(j + 1) * depth].astype(F32)
        ssq = ssq + jnp.sum(v * v, axis=1, keepdims=True)
    scale = lax.rsqrt(ssq / width + 1e-06)
    for j in range(n):
        cs = slice(j * depth, (j + 1) * depth)
        normed[j] = (tokens[:, cs].astype(F32) * scale * mix_gain[:, cs].astype(F32)).astype(BF16)

    pl.semaphore_wait(barrier, n + p - 2)

    def copy_a(d):
        peer = lax.rem(e + d, n)
        return remote(normed.at[peer], cols.at[e], sa.at[d], ra.at[d], {"ep": peer})

    @pl.loop(1, n)
    def _(d):
        copy_a(d).start()

    ids = routes[...]
    lane_e = lax.broadcasted_iota(jnp.int32, (rows_g, n), 1)
    named = [(ids[:, k:k + 1] == lane_e).astype(F32) for k in range(ids.shape[1])]
    member = functools.reduce(lambda a, b: a + b, named)
    earlier = (
        lax.broadcasted_iota(jnp.int32, (rows_g, rows_g), 1)
        < lax.broadcasted_iota(jnp.int32, (rows_g, rows_g), 0)
    ).astype(F32)
    before = dot(earlier.astype(BF16), member.astype(BF16))
    lane_s = lax.broadcasted_iota(jnp.int32, (rows_g, slots), 1).astype(F32)
    total_prob = jnp.sum(prob[...], axis=1, keepdims=True)
    dispatch = jnp.zeros((rows_g, slots), F32)
    comb = jnp.zeros((rows_g, slots), F32)
    for k in range(ids.shape[1]):
        slot = jnp.sum(before * named[k], axis=1, keepdims=True)
        target = ids[:, k:k + 1].astype(F32) * cap + slot
        hit = (lane_s == target).astype(F32)
        dispatch = dispatch + hit
        comb = comb + hit * (prob[:, k:k + 1] / total_prob)
    dispatch = dispatch.astype(BF16)
    comb_hi = comb.astype(BF16)
    comb_lo = (comb - comb_hi.astype(F32)).astype(BF16)

    loads[0].wait()
    loads[1].wait()
    rbuf[e, :, :chans] = dot(normed[e], wr[...]).astype(BF16)
    rbuf[e, :, chans:] = dot(normed[e], wg[...]).astype(BF16)

    def copy_b(d):
        peer = lax.rem(e - d + n, n)
        return remote(part.at[d], rbuf.at[e], sb.at[d], rb.at[d], {"ep": peer})

    @pl.loop(1, n)
    def _(d):
        src = lax.rem(e - d + n, n)
        copy_a(d).wait_recv()
        part[d, :, :chans] = dot(cols[src], wr[...]).astype(BF16)
        part[d, :, chans:] = dot(cols[src], wg[...]).astype(BF16)
        copy_b(d).start()

    @pl.loop(1, n)
    def _(d):
        copy_b(d).wait_recv()

    loads[2].wait()
    loads[3].wait()
    bw = rate_h.shape[1]
    for b in range(rate_h.shape[0]):
        cs = slice(b * bw, (b + 1) * bw)
        cy = slice(chans + b * bw, chans + (b + 1) * bw)
        proj_x = rbuf[0, :, cs].astype(F32)
        proj_y = rbuf[0, :, cy].astype(F32)
        for j in range(1, n):
            proj_x = proj_x + rbuf[j, :, cs].astype(F32)
            proj_y = proj_y + rbuf[j, :, cy].astype(F32)
        moved = proj_x.astype(BF16)
        moved_out[:, cs] = moved
        taps = conv_w[:, cs].astype(F32)
        conv = (hist[:, cs] + moved.astype(F32) * taps[3:4]).astype(BF16)
        rate = jax.nn.sigmoid(dot(conv, wrate[b]))
        in_gate = jax.nn.sigmoid(dot(conv, winput[b]))
        log_decay = -8.0 * rate * jnp.log1p(jnp.exp(-rate_param[:, cs]))
        th = jnp.tanh(log_decay)
        rest = -2.0 * th / (1.0 - th)
        state = jnp.exp(log_decay) * state_in[:, cs] + jnp.sqrt(rest) * in_gate * conv.astype(F32)
        state_out[:, cs] = state
        gated[:, cs] = (state * jax.nn.gelu(proj_y, approximate=True)).astype(BF16)

    def block(i):
        return pl.ds(pl.multiple_of(i * share, share), share)

    loads[4].wait()

    def copy_d1(yy):
        return remote(op_p.at[yy], op_r.at[yy], sd1.at[yy], rd1.at[yy], {"tp": q})

    def copy_d2(dy):
        ty = lax.rem(y + dy, ys)
        return remote(hs.at[ty], hr.at[y], sd2.at[dy], rd2.at[dy], {"tp": ty * 2 + core})

    for dy in range(ys):
        yy = lax.rem(y + dy + 1, ys)
        op_p[yy] = dot(gated[...], wout[:, block(yy * 2 + 1 - core)]).astype(BF16)
        copy_d1(yy).start()
    for dy in range(ys):
        yy = lax.rem(y + dy + 1, ys)
        op_o[yy] = dot(gated[...], wout[:, block(yy * 2 + core)])
    for dy in range(1, ys):
        ty = lax.rem(y + dy, ys)
        copy_d1(ty).wait_recv()
        hs[ty] = (op_o[ty] + op_r[ty].astype(F32)).astype(BF16)
        copy_d2(dy).start()
    copy_d1(y).wait_recv()
    total = tokens[:, block(t)].astype(F32) + op_o[y] + op_r[y].astype(F32)
    for dy in range(1, ys):
        copy_d2(dy).wait_recv()
        total = total + hr[lax.rem(y - dy + ys, ys)].astype(F32)
    mixed[...] = total

    sent = lax.dot_general(
        dispatch, mixed[...].astype(BF16), (((0,), (0,)), ((), ())), preferred_element_type=F32
    )
    sd[...] = sent.reshape(n, cap, share).astype(BF16)

    def copy_c1(d):
        peer = lax.rem(e + d, n)
        return remote(sd.at[peer], rows.at[t, e], sc1.at[d], rc1.at[d], {"ep": peer})

    def copy_c2(dy, d):
        src = lax.rem(e - d + n, n)
        to = lax.rem(y + dy, ys) * 2 + core
        return remote(rows.at[t, src], rows.at[t, src], sc2.at[dy, d], rc2.at[dy, d], {"tp": to})

    def copy_c3(dy, d):
        src = lax.rem(e - d + n, n)
        held = lax.rem(y - dy + ys, ys) * 2 + core
        return remote(rows.at[held, src], rows.at[held, src], sc3.at[dy, d], rc3.at[dy, d], {"tp": q})

    @pl.loop(1, n)
    def _(d):
        copy_c1(d).start()

    rows[t, e] = sd[e]

    def spread(d):
        for dy in range(1, ys):
            copy_c2(dy, d).start()
        copy_c3(0, d).start()

    spread(0)

    @pl.loop(1, n)
    def _(d):
        copy_c1(d).wait_recv()
        spread(d)

    @pl.loop(0, n)
    def _(d):
        for dy in range(1, ys):
            copy_c2(dy, d).wait_recv()
            copy_c3(dy, d).start()

    @pl.loop(0, n)
    def _(d):
        for dy in range(ys):
            copy_c3(dy, d).wait_recv()

    gs = min(n, max(1, 64 // cap))
    span = gs * cap

    @pl.loop(0, n // gs)
    def _(g):
        def piece(i):
            return rows[i, pl.ds(g * gs, gs)].astype(F32).reshape(span, share)

        acc = jnp.zeros((span, 1), F32)
        for i in range(p):
            v = piece(i)
            acc = acc + jnp.sum(v * v, axis=1, keepdims=True)
        sc = lax.rsqrt(acc / width + 1e-06)
        for i in range(p):
            cs = slice(i * share, (i + 1) * share)
            xn[pl.ds(pl.multiple_of(g * span, span), span), cs] = (
                piece(i) * sc * moe_gain[:, cs].astype(F32)
            ).astype(BF16)

    loads[5].wait()
    loads[6].wait()
    hidden = hid.shape[1]
    fc = min(256, hidden)

    @pl.loop(0, hidden // fc)
    def _(c):
        cs = pl.ds(pl.multiple_of(c * fc, fc), fc)
        gate_part = dot(xn[...], weg[:, cs])
        up_part = dot(xn[...], weu[:, cs])
        hid[:, cs] = (jax.nn.silu(gate_part) * up_part).astype(BF16)

    loads[7].wait()

    def copy_e1(yy):
        return remote(e_p.at[yy], e_r.at[yy], se1.at[yy], re1.at[yy], {"tp": q})

    def copy_e2(dy):
        ty = lax.rem(y + dy, ys)
        return remote(es.at[ty], er.at[y], se2.at[dy], re2.at[dy], {"tp": ty * 2 + core})

    def copy_e3(d):
        peer = lax.rem(e + d, n)
        return remote(outb.at[peer], ret.at[e], se3.at[d], re3.at[d], {"ep": peer})

    nc = min(256, share)

    def down(yy, parity, dst):
        @pl.loop(0, share // nc)
        def _(c):
            at = pl.ds(pl.multiple_of((yy * 2 + parity) * share + c * nc, nc), nc)
            dst[yy, :, pl.ds(pl.multiple_of(c * nc, nc), nc)] = dot(hid[...], wed[:, at]).astype(dst.dtype)

    for dy in range(ys):
        yy = lax.rem(y + dy + 1, ys)
        down(yy, 1 - core, e_p)
        copy_e1(yy).start()
    for dy in range(ys):
        down(lax.rem(y + dy + 1, ys), core, e_o)
    for dy in range(1, ys):
        ty = lax.rem(y + dy, ys)
        copy_e1(ty).wait_recv()
        es[ty] = (e_o[ty] + e_r[ty].astype(F32)).astype(BF16)
        copy_e2(dy).start()
    copy_e1(y).wait_recv()
    for dy in range(1, ys):
        copy_e2(dy).wait_recv()
    result = e_o[y] + e_r[y].astype(F32)
    for dy in range(1, ys):
        result = result + er[lax.rem(y - dy + ys, ys)].astype(F32)
    outb[...] = result.reshape(n, cap, share).astype(BF16)

    @pl.loop(1, n)
    def _(d):
        copy_e3(d).start()

    ret[e] = outb[e]

    @pl.loop(1, n)
    def _(d):
        copy_e3(d).wait_recv()

    back = ret[...].astype(F32).reshape(slots, share).astype(BF16)
    layer_out[...] = (mixed[...] + dot(comb_hi, back) + dot(comb_lo, back)).astype(BF16)

    @pl.loop(1, n)
    def _(d):
        copy_a(d).wait_send()
        copy_b(d).wait_send()
        copy_c1(d).wait_send()
        copy_e3(d).wait_send()

    @pl.loop(0, n)
    def _(d):
        for dy in range(1, ys):
            copy_c2(dy, d).wait_send()
        for dy in range(ys):
            copy_c3(dy, d).wait_send()

    for dy in range(ys):
        copy_d1(dy).wait_send()
        copy_e1(dy).wait_send()
    for dy in range(1, ys):
        copy_d2(dy).wait_send()
        copy_e2(dy).wait_send()


def shards(
    n, p,
    tokens, state_in, conv_in, mix_gain, rnn_weight, gate_weight, conv_weight, rate_weight,
    input_weight, rate_param, out_weight, moe_gain, expert_gate, expert_up, expert_down, routes, route_prob,
):
    g, width = tokens.shape
    depth, chans = rnn_weight.shape
    share = width // p
    cap = max(2, 2 * g * routes.shape[1] // n)
    slots = n * cap
    hidden = expert_gate.shape[2]
    ys = p // 2
    taps = conv_weight.astype(F32)
    history = conv_in.astype(F32)
    hist = history[:, 0] * taps[0] + history[:, 1] * taps[1] + history[:, 2] * taps[2]
    vm = pl.BlockSpec(memory_space=pltpu.VMEM)
    hb = pl.BlockSpec(memory_space=pl.ANY)
    dma = pltpu.SemaphoreType.DMA
    V = pltpu.VMEM
    scratch = [
        V((depth, chans), BF16), V((depth, chans), BF16),
        V(rate_weight.shape, BF16), V(input_weight.shape, BF16), V(out_weight.shape, BF16),
        V(expert_gate.shape[1:], BF16), V(expert_up.shape[1:], BF16), V(expert_down.shape[1:], BF16),
        V((n, g, depth), BF16), V((n, g, depth), BF16), V((n, g, 2 * chans), BF16), V((n, g, 2 * chans), BF16),
        V((g, chans), BF16),
        V((ys, g, share), BF16), V((ys, g, share), F32), V((ys, g, share), BF16),
        V((ys, g, share), BF16), V((ys, g, share), BF16), V((g, share), F32),
        V((n, cap, share), BF16), V((p, n, cap, share), BF16), V((slots, width), BF16), V((slots, hidden), BF16),
        V((ys, slots, share), BF16), V((ys, slots, share), F32), V((ys, slots, share), BF16),
        V((ys, slots, share), BF16), V((ys, slots, share), BF16),
        V((n, cap, share), BF16), V((n, cap, share), BF16),
        dma((8,)),
        dma((n,)), dma((n,)), dma((n,)), dma((n,)),
        dma((ys,)), dma((ys,)), dma((ys,)), dma((ys,)),
        dma((n,)), dma((n,)), dma((ys, n)), dma((ys, n)), dma((ys, n)), dma((ys, n)),
        dma((ys,)), dma((ys,)), dma((ys,)), dma((ys,)), dma((n,)), dma((n,)),
    ]
    layer_out, state_out, moved = pl.pallas_call(
        functools.partial(kernel, n, p, cap),
        out_shape=(
            jax.ShapeDtypeStruct((g, share), BF16),
            jax.ShapeDtypeStruct((g, chans), F32),
            jax.ShapeDtypeStruct((g, chans), BF16),
        ),
        in_specs=[vm] * 9 + [hb] * 8,
        out_specs=(vm, vm, vm),
        scratch_shapes=scratch,
        compiler_params=pltpu.CompilerParams(
            collective_id=0, has_side_effects=True, vmem_limit_bytes=60 * 1024 * 1024
        ),
    )(
        tokens, state_in, hist, mix_gain[None], moe_gain[None], conv_weight, rate_param[None], routes, route_prob,
        rnn_weight, gate_weight, rate_weight, input_weight, out_weight, expert_gate, expert_up, expert_down,
    )
    conv_out = jnp.concatenate([conv_in[:, 1:], moved[:, None, :]], axis=1)
    return (layer_out, state_out, conv_out)


def solution(mesh):
    in_specs = (
        P("ep", None),
        P("ep", "tp"),
        P("ep", None, "tp"),
        P(),
        P("ep", "tp"),
        P("ep", "tp"),
        P(None, "tp"),
        P("tp", None, None),
        P("tp", None, None),
        P("tp"),
        P("tp", None),
        P(),
        P("ep", None, "tp"),
        P("ep", None, "tp"),
        P("ep", "tp", None),
        P("ep", None),
        P("ep", None),
    )
    out_specs = (P("ep", "tp"), P("ep", "tp"), P("ep", None, "tp"))
    body = functools.partial(shards, mesh.shape["ep"], mesh.shape["tp"])
    return jax.shard_map(body, mesh=mesh, in_specs=in_specs, out_specs=out_specs, check_vma=False)
```

```python
import functools

import jax
import jax.numpy as jnp
from jax import lax
from jax.experimental import pallas as pl
from jax.experimental.pallas import tpu as pltpu
from jax.sharding import PartitionSpec as P

MESH = pl.DeviceIdType.MESH
F32 = jnp.float32
BF16 = jnp.bfloat16


def dot(a, b):
    return jnp.dot(a, b, preferred_element_type=F32)


def remote(src, dst, send, recv, where):
    return pltpu.make_async_remote_copy(
        src_ref=src, dst_ref=dst, send_sem=send, recv_sem=recv, device_id=where, device_id_type=MESH
    )


def kernel(
    n, p, nx, cap,
    tokens, state_in, conv_in, mix_gain_in, moe_gain_in, conv_w, rate_param, routes, prob,
    rnn_h, gate_h, rate_h, input_h, out_h, eg_h, eu_h, ed_h,
    layer_out, state_out, moved_out,
    wr, wg, wrate, winput, wout, weg, weu, wed,
    mix_gain, moe_gain, normed, cols, part, bx, zsend, rbuf, gated,
    op_p, op_o, op_r, hs, hr, mixed,
    sd, rows, xn, hid, e_p, e_o, e_r, es, er, outb, ret,
    wsem, sa, ra, sa2, ra2, sb, rb, sbz, rbz, sd1, rd1, sd2, rd2, sc1, rc1, sc2, rc2, sc3, rc3,
    se1, re1, se2, re2, se3, re3,
):
    e = lax.axis_index("ep")
    t = lax.axis_index("tp")
    core = lax.rem(t, 2)
    y = t // 2
    q = t + 1 - 2 * core
    ys = p // 2
    nz = n // nx
    z = e // nx
    x = lax.rem(e, nx)
    far_first = sorted(range(nz), key=lambda dz: -min(dz, nz - dz))

    def up(d):
        return lax.rem(z + d // nx, nz) * nx + lax.rem(x + d % nx, nx)

    def down_of(d):
        return lax.rem(z - d // nx + nz, nz) * nx + lax.rem(x - d % nx + nx, nx)

    rows_g, width = tokens.shape
    depth = width // n
    chans = rnn_h.shape[1]
    share = width // p
    slots = n * cap

    loads = [
        pltpu.make_async_copy(a, b, wsem.at[i])
        for i, (a, b) in enumerate(
            [(rnn_h, wr), (gate_h, wg), (rate_h, wrate), (input_h, winput), (out_h, wout),
             (eg_h.at[0], weg), (eu_h.at[0], weu), (ed_h.at[0], wed)]
        )
    ]
    for load in loads:
        load.start()

    barrier = pltpu.get_barrier_semaphore()

    @pl.loop(1, n)
    def _(d):
        pl.semaphore_signal(barrier, inc=1, device_id={"ep": lax.rem(e + d, n)}, device_id_type=MESH)

    @pl.loop(1, p)
    def _(d):
        pl.semaphore_signal(barrier, inc=1, device_id={"tp": lax.rem(t + d, p)}, device_id_type=MESH)

    for j in range(width // 128):
        cs = slice(j * 128, (j + 1) * 128)
        mix_gain[:, cs] = mix_gain_in[j:j + 1, :].astype(F32)
        moe_gain[:, cs] = moe_gain_in[j:j + 1, :].astype(F32)

    ssq = jnp.zeros((rows_g, 1), F32)
    for j in range(n):
        v = tokens[:, j * depth:(j + 1) * depth].astype(F32)
        ssq = ssq + jnp.sum(v * v, axis=1, keepdims=True)
    scale = lax.rsqrt(ssq / width + 1e-06)
    for j in range(n):
        cs = slice(j * depth, (j + 1) * depth)
        normed[j] = (tokens[:, cs].astype(F32) * scale * mix_gain[:, cs]).astype(BF16)

    pl.semaphore_wait(barrier, n + p - 2)

    half = pl.ds(pl.multiple_of(core * (rows_g // 2), rows_g // 2), rows_g // 2)

    def copy_a(d):
        peer = up(d)
        return remote(normed.at[peer, half], cols.at[e, half], sa.at[d], ra.at[d], {"ep": peer})

    def copy_a2(d):
        src = down_of(d)
        return remote(cols.at[src, half], cols.at[src, half], sa2.at[d], ra2.at[d], {"tp": q})

    for d in range(1, n):
        copy_a(d).start()
    cols[e] = normed[e]

    ids = routes[...]
    sub_e = lax.broadcasted_iota(jnp.int32, (n, rows_g), 0)
    named = [(ids[k:k + 1, :] == sub_e).astype(F32) for k in range(ids.shape[0])]
    member = functools.reduce(lambda a, b: a + b, named)
    earlier = (
        lax.broadcasted_iota(jnp.int32, (rows_g, rows_g), 0)
        < lax.broadcasted_iota(jnp.int32, (rows_g, rows_g), 1)
    ).astype(F32)
    before = dot(member.astype(BF16), earlier.astype(BF16))
    sub_s = lax.broadcasted_iota(jnp.int32, (slots, rows_g), 0).astype(F32)
    total_prob = jnp.sum(prob[...], axis=0, keepdims=True)
    dispatch = jnp.zeros((slots, rows_g), F32)
    comb = jnp.zeros((slots, rows_g), F32)
    for k in range(ids.shape[0]):
        slot = jnp.sum(before * named[k], axis=0, keepdims=True)
        target = ids[k:k + 1, :].astype(F32) * cap + slot
        hit = (sub_s == target).astype(F32)
        dispatch = dispatch + hit
        comb = comb + hit * (prob[k:k + 1, :] / total_prob)
    dispatch = dispatch.astype(BF16)
    comb_hi = comb.astype(BF16)
    comb_lo = (comb - comb_hi.astype(F32)).astype(BF16)

    loads[0].wait()
    loads[1].wait()

    def copy_b(dz, dx):
        zs = lax.rem(z - dz + nz, nz)
        peer = z * nx + lax.rem(x - dx + nx, nx)
        return remote(part.at[dz, dx], bx.at[dz, dx], sb.at[dz, dx], rb.at[dz, dx], {"ep": peer})

    def copy_bz(dz):
        peer = lax.rem(z - dz + nz, nz) * nx + x
        return remote(zsend.at[dz], rbuf.at[dz], sbz.at[dz], rbz.at[dz], {"ep": peer})

    def pass_on(dz):
        for lo in (0, chans):
            cs = slice(lo, lo + chans)
            if lo == 0:
                for dx in range(1, nx):
                    copy_b(dz, dx).wait_recv()
            acc = part[dz, 0, :, cs].astype(F32)
            for dx in range(1, nx):
                acc = acc + bx[dz, dx, :, cs].astype(F32)
            if dz:
                zsend[dz, :, cs] = acc.astype(BF16)
            else:
                rbuf[0, :, cs] = acc.astype(BF16)
        if dz:
            copy_bz(dz).start()

    for dz in range(nz):
        for dx in range(nx):
            d = dz * nx + dx
            if d:
                copy_a(d).wait_recv()
                copy_a2(d).start()
        for dx in list(range(1, nx)) + [0]:
            d = dz * nx + dx
            if d:
                copy_a2(d).wait_recv()
            src = down_of(d)
            part[dz, dx, :, :chans] = dot(cols[src], wr[...]).astype(BF16)
            part[dz, dx, :, chans:] = dot(cols[src], wg[...]).astype(BF16)
            if dx:
                copy_b(dz, dx).start()
        if dz >= 2:
            pass_on(dz - 1)
    pass_on(nz - 1)
    pass_on(0)
    for dz in range(1, nz):
        copy_bz(dz).wait_recv()

    loads[2].wait()
    loads[3].wait()
    bw = rate_h.shape[1]
    for b in range(rate_h.shape[0]):
        cs = slice(b * bw, (b + 1) * bw)
        cy = slice(chans + b * bw, chans + (b + 1) * bw)
        proj_x = rbuf[0, :, cs].astype(F32)
        proj_y = rbuf[0, :, cy].astype(F32)
        for j in range(1, nz):
            proj_x = proj_x + rbuf[j, :, cs].astype(F32)
            proj_y = proj_y + rbuf[j, :, cy].astype(F32)
        moved = proj_x.astype(BF16)
        moved_out[:, cs] = moved
        taps = conv_w[:, cs].astype(F32)
        hist = conv_in[0, :, cs].astype(F32) * taps[0:1]
        for i in range(1, 3):
            hist = hist + conv_in[i, :, cs].astype(F32) * taps[i:i + 1]
        conv = (hist + moved.astype(F32) * taps[3:4]).astype(BF16)
        rate = jax.nn.sigmoid(dot(conv, wrate[b]))
        in_gate = jax.nn.sigmoid(dot(conv, winput[b]))
        log_decay = -8.0 * rate * jnp.log1p(jnp.exp(-rate_param[:, cs]))
        th = jnp.tanh(log_decay)
        rest = -2.0 * th / (1.0 - th)
        state = jnp.exp(log_decay) * state_in[:, cs] + jnp.sqrt(rest) * in_gate * conv.astype(F32)
        state_out[:, cs] = state
        gated[:, cs] = (state * jax.nn.gelu(proj_y, approximate=True)).astype(BF16)

    def block(i):
        return pl.ds(pl.multiple_of(i * share, share), share)

    loads[4].wait()

    def copy_d1(yy):
        return remote(op_p.at[yy], op_r.at[yy], sd1.at[yy], rd1.at[yy], {"tp": q})

    def copy_d2(dy):
        ty = lax.rem(y + dy, ys)
        return remote(hs.at[ty], hr.at[y], sd2.at[dy], rd2.at[dy], {"tp": ty * 2 + core})

    for dy in range(ys):
        yy = lax.rem(y + dy + 1, ys)
        op_p[yy] = dot(gated[...], wout[:, block(yy * 2 + 1 - core)]).astype(BF16)
        copy_d1(yy).start()
    for dy in range(ys):
        yy = lax.rem(y + dy + 1, ys)
        op_o[yy] = dot(gated[...], wout[:, block(yy * 2 + core)])
    for dy in range(1, ys):
        ty = lax.rem(y + dy, ys)
        copy_d1(ty).wait_recv()
        hs[ty] = (op_o[ty] + op_r[ty].astype(F32)).astype(BF16)
        copy_d2(dy).start()
    copy_d1(y).wait_recv()
    total = tokens[:, block(t)].astype(F32) + op_o[y] + op_r[y].astype(F32)
    for dy in range(1, ys):
        copy_d2(dy).wait_recv()
        total = total + hr[lax.rem(y - dy + ys, ys)].astype(F32)
    mixed[...] = total

    sent = dot(dispatch, mixed[...].astype(BF16))
    sd[...] = sent.reshape(n, cap, share).astype(BF16)

    def copy_c1(d):
        peer = up(d)
        return remote(sd.at[peer], rows.at[t, e], sc1.at[d], rc1.at[d], {"ep": peer})

    def copy_c2(dy, d):
        src = down_of(d)
        to = lax.rem(y + dy, ys) * 2 + core
        return remote(rows.at[t, src], rows.at[t, src], sc2.at[dy, d], rc2.at[dy, d], {"tp": to})

    def copy_c3(dy, d):
        src = down_of(d)
        held = lax.rem(y - dy + ys, ys) * 2 + core
        return remote(rows.at[held, src], rows.at[held, src], sc3.at[dy, d], rc3.at[dy, d], {"tp": q})

    order = [dz * nx + dx for dz in far_first for dx in range(nx) if dz + dx]
    for d in order:
        copy_c1(d).start()

    rows[t, e] = sd[e]

    def spread(d):
        for dy in range(1, ys):
            copy_c2(dy, d).start()
        copy_c3(0, d).start()

    def relay(d):
        for dy in range(1, ys):
            copy_c2(dy, d).wait_recv()
            copy_c3(dy, d).start()

    near = order[::-1]
    spread(0)
    for i, d in enumerate(near):
        copy_c1(d).wait_recv()
        spread(d)
        if i >= 1:
            relay(([0] + near)[i - 1])
    for d in ([0] + near)[len(near) - 1:]:
        relay(d)
    for d in range(n):
        for dy in range(ys):
            copy_c3(dy, d).wait_recv()

    gs = min(n, max(1, 64 // cap))
    span = gs * cap

    @pl.loop(0, n // gs)
    def _(g):
        def piece(i):
            return rows[i, pl.ds(g * gs, gs)].astype(F32).reshape(span, share)

        acc = jnp.zeros((span, 1), F32)
        for i in range(p):
            v = piece(i)
            acc = acc + jnp.sum(v * v, axis=1, keepdims=True)
        sc = lax.rsqrt(acc / width + 1e-06)
        for i in range(p):
            cs = slice(i * share, (i + 1) * share)
            xn[pl.ds(pl.multiple_of(g * span, span), span), cs] = (
                piece(i) * sc * moe_gain[:, cs]
            ).astype(BF16)

    loads[5].wait()
    loads[6].wait()
    hidden = hid.shape[1]
    fc = min(256, hidden)

    @pl.loop(0, hidden // fc)
    def _(c):
        cs = pl.ds(pl.multiple_of(c * fc, fc), fc)
        gate_part = dot(xn[...], weg[:, cs])
        up_part = dot(xn[...], weu[:, cs])
        hid[:, cs] = (jax.nn.silu(gate_part) * up_part).astype(BF16)

    loads[7].wait()

    def copy_e1(yy):
        return remote(e_p.at[yy], e_r.at[yy], se1.at[yy], re1.at[yy], {"tp": q})

    def copy_e2(dy, dz):
        ty = lax.rem(y + dy, ys)
        zc = lax.rem(z + dz, nz)
        return remote(
            es.at[ty, zc], er.at[y, zc], se2.at[dy, dz], re2.at[dy, dz], {"tp": ty * 2 + core}
        )

    def copy_e3(d):
        peer = up(d)
        return remote(outb.at[peer], ret.at[e], se3.at[d], re3.at[d], {"ep": peer})

    nc = min(256, share)
    chunk = nx * cap

    def down(yy, parity, dst):
        @pl.loop(0, share // nc)
        def _(c):
            at = pl.ds(pl.multiple_of((yy * 2 + parity) * share + c * nc, nc), nc)
            value = dot(hid[...], wed[:, at]).reshape(nz, chunk, nc)
            dst[yy, :, :, pl.ds(pl.multiple_of(c * nc, nc), nc)] = value.astype(dst.dtype)

    for dy in list(range(1, ys)) + [0]:
        ty = lax.rem(y + dy, ys)
        down(ty, 1 - core, e_p)
        copy_e1(ty).start()
        down(ty, core, e_o)
        copy_e1(ty).wait_recv()
        if dy:
            for dz in far_first:
                zc = lax.rem(z + dz, nz)
                es[ty, zc] = (e_o[ty, zc] + e_r[ty, zc].astype(F32)).astype(BF16)
                copy_e2(dy, dz).start()
    for dz in far_first:
        zc = lax.rem(z + dz, nz)
        result = e_o[y, zc] + e_r[y, zc].astype(F32)
        for dy in range(1, ys):
            copy_e2(dy, dz).wait_recv()
            result = result + er[lax.rem(y - dy + ys, ys), zc].astype(F32)
        outb[pl.ds(zc * nx, nx)] = result.reshape(nx, cap, share).astype(BF16)
        for dx in range(nx):
            if dz + dx:
                copy_e3(dz * nx + dx).start()

    ret[e] = outb[e]
    for d in order:
        copy_e3(d).wait_recv()

    back = ret[...].astype(F32).reshape(slots, share).astype(BF16)

    def combine(weights):
        return lax.dot_general(weights, back, (((0,), (0,)), ((), ())), preferred_element_type=F32)

    layer_out[...] = (mixed[...] + combine(comb_hi) + combine(comb_lo)).astype(BF16)

    @pl.loop(1, n)
    def _(d):
        copy_a(d).wait_send()
        copy_a2(d).wait_send()
        copy_c1(d).wait_send()
        copy_e3(d).wait_send()

    @pl.loop(0, n)
    def _(d):
        for dy in range(1, ys):
            copy_c2(dy, d).wait_send()
        for dy in range(ys):
            copy_c3(dy, d).wait_send()

    for dy in range(ys):
        copy_d1(dy).wait_send()
        copy_e1(dy).wait_send()
    for dy in range(1, ys):
        copy_d2(dy).wait_send()
        for dz in range(nz):
            copy_e2(dy, dz).wait_send()
    for dz in range(nz):
        for dx in range(1, nx):
            copy_b(dz, dx).wait_send()
        if dz:
            copy_bz(dz).wait_send()


def finish(layer_in, state_in, moved, conv_in, layer_out, state_out, conv_out):
    layer_out[...] = layer_in[...]
    state_out[...] = state_in[...]
    kept = conv_in.shape[0] - 1
    for i in range(kept):
        conv_out[i] = conv_in[i + 1]
    conv_out[kept] = moved[...]


def shards(
    n, p,
    tokens, state_in, conv_in, mix_gain, rnn_weight, gate_weight, conv_weight, rate_weight,
    input_weight, rate_param, out_weight, moe_gain, expert_gate, expert_up, expert_down, routes, route_prob,
):
    g, width = tokens.shape
    depth, chans = rnn_weight.shape
    share = width // p
    cap = max(2, 2 * g * routes.shape[1] // n)
    slots = n * cap
    hidden = expert_gate.shape[2]
    ys = p // 2
    nx = 1 << ((n.bit_length() - 1) // 2)
    nx = nx if n % nx == 0 else 1
    nz = n // nx
    conv_t = jnp.transpose(conv_in, (1, 0, 2))
    vm = pl.BlockSpec(memory_space=pltpu.VMEM)
    hb = pl.BlockSpec(memory_space=pl.ANY)
    dma = pltpu.SemaphoreType.DMA
    V = pltpu.VMEM
    scratch = [
        V((depth, chans), BF16), V((depth, chans), BF16),
        V(rate_weight.shape, BF16), V(input_weight.shape, BF16), V(out_weight.shape, BF16),
        V(expert_gate.shape[1:], BF16), V(expert_up.shape[1:], BF16), V(expert_down.shape[1:], BF16),
        V((1, width), F32), V((1, width), F32),
        V((n, g, depth), BF16), V((n, g, depth), BF16),
        V((nz, nx, g, 2 * chans), BF16), V((nz, nx, g, 2 * chans), BF16),
        V((nz, g, 2 * chans), BF16), V((nz, g, 2 * chans), BF16),
        V((g, chans), BF16),
        V((ys, g, share), BF16), V((ys, g, share), F32), V((ys, g, share), BF16),
        V((ys, g, share), BF16), V((ys, g, share), BF16), V((g, share), F32),
        V((n, cap, share), BF16), V((p, n, cap, share), BF16), V((slots, width), BF16), V((slots, hidden), BF16),
        V((ys, nz, nx * cap, share), BF16), V((ys, nz, nx * cap, share), F32), V((ys, nz, nx * cap, share), BF16),
        V((ys, nz, nx * cap, share), BF16), V((ys, nz, nx * cap, share), BF16),
        V((n, cap, share), BF16), V((n, cap, share), BF16),
        dma((8,)),
        dma((n,)), dma((n,)), dma((n,)), dma((n,)), dma((nz, nx)), dma((nz, nx)), dma((nz,)), dma((nz,)),
        dma((ys,)), dma((ys,)), dma((ys,)), dma((ys,)),
        dma((n,)), dma((n,)), dma((ys, n)), dma((ys, n)), dma((ys, n)), dma((ys, n)),
        dma((ys,)), dma((ys,)), dma((ys, nz)), dma((ys, nz)), dma((n,)), dma((n,)),
    ]
    layer, state, moved = pl.pallas_call(
        functools.partial(kernel, n, p, nx, cap),
        out_shape=(
            jax.ShapeDtypeStruct((g, share), BF16),
            jax.ShapeDtypeStruct((g, chans), F32),
            jax.ShapeDtypeStruct((g, chans), BF16),
        ),
        in_specs=[vm] * 9 + [hb] * 8,
        out_specs=(vm, vm, vm),
        scratch_shapes=scratch,
        compiler_params=pltpu.CompilerParams(
            collective_id=0, has_side_effects=True, vmem_limit_bytes=60 * 1024 * 1024
        ),
    )(
        tokens, state_in, conv_t, mix_gain.reshape(-1, 128), moe_gain.reshape(-1, 128),
        conv_weight, rate_param[None], routes.T, route_prob.T,
        rnn_weight, gate_weight, rate_weight, input_weight, out_weight, expert_gate, expert_up, expert_down,
    )
    layer_out, state_out, conv_out = pl.pallas_call(
        finish,
        out_shape=(
            jax.ShapeDtypeStruct(layer.shape, layer.dtype),
            jax.ShapeDtypeStruct(state.shape, state.dtype),
            jax.ShapeDtypeStruct(conv_t.shape, conv_t.dtype),
        ),
        in_specs=[vm] * 4,
        out_specs=(vm, vm, vm),
    )(layer, state, moved, conv_t)
    return (layer_out, state_out, jnp.transpose(conv_out, (1, 0, 2)))


def solution(mesh):
    in_specs = (
        P("ep", None),
        P("ep", "tp"),
        P("ep", None, "tp"),
        P(),
        P("ep", "tp"),
        P("ep", "tp"),
        P(None, "tp"),
        P("tp", None, None),
        P("tp", None, None),
        P("tp"),
        P("tp", None),
        P(),
        P("ep", None, "tp"),
        P("ep", None, "tp"),
        P("ep", "tp", None),
        P("ep", None),
        P("ep", None),
    )
    out_specs = (P("ep", "tp"), P("ep", "tp"), P("ep", None, "tp"))
    body = functools.partial(shards, mesh.shape["ep"], mesh.shape["tp"])
    return jax.shard_map(body, mesh=mesh, in_specs=in_specs, out_specs=out_specs, check_vma=False)
```

```python
import functools

import jax
import jax.numpy as jnp
from jax import lax
from jax.experimental import pallas as pl
from jax.experimental.pallas import tpu as pltpu
from jax.sharding import PartitionSpec as P

MESH = pl.DeviceIdType.MESH
F32 = jnp.float32
BF16 = jnp.bfloat16


def dot(a, b):
    return jnp.dot(a, b, preferred_element_type=F32)


def remote(src, dst, send, recv, where):
    return pltpu.make_async_remote_copy(
        src_ref=src, dst_ref=dst, send_sem=send, recv_sem=recv, device_id=where, device_id_type=MESH
    )


def kernel(
    n, p, nx, cap,
    tokens, state_in, conv_in, mix_gain_in, moe_gain_in, conv_w, rate_param, routes, prob,
    rnn_h, gate_h, rate_h, input_h, out_h, eg_h, eu_h, ed_h,
    layer_out, state_out, moved_out,
    wr, wg, wrate, winput, wout, weg, weu, wed,
    mix_gain, moe_gain, normed, cols, part, bx, zsend, rbuf, gated,
    op_p, op_o, op_r, hs, hr, mixed,
    sd, rows, xn, hid, e_p, e_o, e_r, es, er, outb, ret,
    wsem, sa, ra, sa2, ra2, sb, rb, sbz, rbz, sd1, rd1, sd2, rd2, sc1, rc1, sc2, rc2, sc3, rc3,
    se1, re1, se2, re2, se3, re3,
):
    e = lax.axis_index("ep")
    t = lax.axis_index("tp")
    core = lax.rem(t, 2)
    y = t // 2
    q = t + 1 - 2 * core
    ys = p // 2
    nz = n // nx
    z = e // nx
    x = lax.rem(e, nx)
    far_first = sorted(range(nz), key=lambda dz: -min(dz, nz - dz))

    def up(d):
        return lax.rem(z + d // nx, nz) * nx + lax.rem(x + d % nx, nx)

    def down_of(d):
        return lax.rem(z - d // nx + nz, nz) * nx + lax.rem(x - d % nx + nx, nx)

    rows_g, width = tokens.shape
    depth = width // n
    chans = rnn_h.shape[1]
    share = width // p
    slots = n * cap

    loads = [
        pltpu.make_async_copy(a, b, wsem.at[i])
        for i, (a, b) in enumerate(
            [(rnn_h, wr), (gate_h, wg), (rate_h, wrate), (input_h, winput), (out_h, wout),
             (eg_h.at[0], weg), (eu_h.at[0], weu), (ed_h.at[0], wed)]
        )
    ]
    for load in loads[:4]:
        load.start()

    barrier = pltpu.get_barrier_semaphore()

    @pl.loop(1, n)
    def _(d):
        pl.semaphore_signal(barrier, inc=1, device_id={"ep": lax.rem(e + d, n)}, device_id_type=MESH)

    @pl.loop(1, p)
    def _(d):
        pl.semaphore_signal(barrier, inc=1, device_id={"tp": lax.rem(t + d, p)}, device_id_type=MESH)

    for j in range(width // 128):
        cs = slice(j * 128, (j + 1) * 128)
        mix_gain[:, cs] = mix_gain_in[j:j + 1, :].astype(F32)
        moe_gain[:, cs] = moe_gain_in[j:j + 1, :].astype(F32)

    ssq = jnp.zeros((rows_g, 1), F32)
    for j in range(n):
        v = tokens[:, j * depth:(j + 1) * depth].astype(F32)
        ssq = ssq + jnp.sum(v * v, axis=1, keepdims=True)
    scale = lax.rsqrt(ssq / width + 1e-06)
    for j in range(n):
        cs = slice(j * depth, (j + 1) * depth)
        normed[j] = (tokens[:, cs].astype(F32) * scale * mix_gain[:, cs]).astype(BF16)

    pl.semaphore_wait(barrier, n + p - 2)

    half = pl.ds(pl.multiple_of(core * (rows_g // 2), rows_g // 2), rows_g // 2)

    def copy_a(d):
        peer = up(d)
        return remote(normed.at[peer, half], cols.at[e, half], sa.at[d], ra.at[d], {"ep": peer})

    def copy_a2(d):
        src = down_of(d)
        return remote(cols.at[src, half], cols.at[src, half], sa2.at[d], ra2.at[d], {"tp": q})

    away_first = list(range(1, nz)) + [0]
    for dz in away_first:
        for dx in range(nx):
            if dz + dx:
                copy_a(dz * nx + dx).start()
    cols[e] = normed[e]

    ids = routes[...]
    sub_e = lax.broadcasted_iota(jnp.int32, (n, rows_g), 0)
    named = [(ids[k:k + 1, :] == sub_e).astype(F32) for k in range(ids.shape[0])]
    member = functools.reduce(lambda a, b: a + b, named)
    earlier = (
        lax.broadcasted_iota(jnp.int32, (rows_g, rows_g), 0)
        < lax.broadcasted_iota(jnp.int32, (rows_g, rows_g), 1)
    ).astype(F32)
    before = dot(member.astype(BF16), earlier.astype(BF16))
    sub_s = lax.broadcasted_iota(jnp.int32, (slots, rows_g), 0).astype(F32)
    total_prob = jnp.sum(prob[...], axis=0, keepdims=True)
    dispatch = jnp.zeros((slots, rows_g), F32)
    comb = jnp.zeros((slots, rows_g), F32)
    for k in range(ids.shape[0]):
        slot = jnp.sum(before * named[k], axis=0, keepdims=True)
        target = ids[k:k + 1, :].astype(F32) * cap + slot
        hit = (sub_s == target).astype(F32)
        dispatch = dispatch + hit
        comb = comb + hit * (prob[k:k + 1, :] / total_prob)
    dispatch = dispatch.astype(BF16)
    comb_hi = comb.astype(BF16)
    comb_lo = (comb - comb_hi.astype(F32)).astype(BF16)

    loads[0].wait()
    loads[1].wait()
    for load in loads[4:]:
        load.start()

    def copy_b(dz, dx):
        zs = lax.rem(z - dz + nz, nz)
        peer = z * nx + lax.rem(x - dx + nx, nx)
        return remote(part.at[dz, dx], bx.at[dz, dx], sb.at[dz, dx], rb.at[dz, dx], {"ep": peer})

    def copy_bz(dz):
        peer = lax.rem(z - dz + nz, nz) * nx + x
        return remote(zsend.at[dz], rbuf.at[dz], sbz.at[dz], rbz.at[dz], {"ep": peer})

    def pass_on(dz):
        for lo in (0, chans):
            cs = slice(lo, lo + chans)
            if lo == 0:
                for dx in range(1, nx):
                    copy_b(dz, dx).wait_recv()
            acc = part[dz, 0, :, cs].astype(F32)
            for dx in range(1, nx):
                acc = acc + bx[dz, dx, :, cs].astype(F32)
            if dz:
                zsend[dz, :, cs] = acc.astype(BF16)
            else:
                rbuf[0, :, cs] = acc.astype(BF16)
        if dz:
            copy_bz(dz).start()

    for k, dz in enumerate(away_first):
        for dx in range(nx):
            d = dz * nx + dx
            if d:
                copy_a(d).wait_recv()
                copy_a2(d).start()
        for dx in list(range(1, nx)) + [0]:
            d = dz * nx + dx
            if d:
                copy_a2(d).wait_recv()
            src = down_of(d)
            part[dz, dx, :, :chans] = dot(cols[src], wr[...]).astype(BF16)
            part[dz, dx, :, chans:] = dot(cols[src], wg[...]).astype(BF16)
            if dx:
                copy_b(dz, dx).start()
        if k:
            pass_on(away_first[k - 1])
    pass_on(0)
    for dz in range(1, nz):
        copy_bz(dz).wait_recv()

    loads[2].wait()
    loads[3].wait()
    bw = rate_h.shape[1]
    for b in range(rate_h.shape[0]):
        cs = slice(b * bw, (b + 1) * bw)
        cy = slice(chans + b * bw, chans + (b + 1) * bw)
        proj_x = rbuf[0, :, cs].astype(F32)
        proj_y = rbuf[0, :, cy].astype(F32)
        for j in range(1, nz):
            proj_x = proj_x + rbuf[j, :, cs].astype(F32)
            proj_y = proj_y + rbuf[j, :, cy].astype(F32)
        moved = proj_x.astype(BF16)
        moved_out[:, cs] = moved
        taps = conv_w[:, cs].astype(F32)
        hist = conv_in[0, :, cs].astype(F32) * taps[0:1]
        for i in range(1, 3):
            hist = hist + conv_in[i, :, cs].astype(F32) * taps[i:i + 1]
        conv = (hist + moved.astype(F32) * taps[3:4]).astype(BF16)
        rate = jax.nn.sigmoid(dot(conv, wrate[b]))
        in_gate = jax.nn.sigmoid(dot(conv, winput[b]))
        log_decay = -8.0 * rate * jnp.log1p(jnp.exp(-rate_param[:, cs]))
        th = jnp.tanh(log_decay)
        rest = -2.0 * th / (1.0 - th)
        state = jnp.exp(log_decay) * state_in[:, cs] + jnp.sqrt(rest) * in_gate * conv.astype(F32)
        state_out[:, cs] = state
        gated[:, cs] = (state * jax.nn.gelu(proj_y, approximate=True)).astype(BF16)

    def block(i):
        return pl.ds(pl.multiple_of(i * share, share), share)

    loads[4].wait()

    def copy_d1(yy):
        return remote(op_p.at[yy], op_r.at[yy], sd1.at[yy], rd1.at[yy], {"tp": q})

    def copy_d2(dy):
        ty = lax.rem(y + dy, ys)
        return remote(hs.at[ty], hr.at[y], sd2.at[dy], rd2.at[dy], {"tp": ty * 2 + core})

    for dy in range(ys):
        yy = lax.rem(y + dy + 1, ys)
        op_p[yy] = dot(gated[...], wout[:, block(yy * 2 + 1 - core)]).astype(BF16)
        copy_d1(yy).start()
    for dy in range(ys):
        yy = lax.rem(y + dy + 1, ys)
        op_o[yy] = dot(gated[...], wout[:, block(yy * 2 + core)])
    for dy in range(1, ys):
        ty = lax.rem(y + dy, ys)
        copy_d1(ty).wait_recv()
        hs[ty] = (op_o[ty] + op_r[ty].astype(F32)).astype(BF16)
        copy_d2(dy).start()
    copy_d1(y).wait_recv()
    total = tokens[:, block(t)].astype(F32) + op_o[y] + op_r[y].astype(F32)
    for dy in range(1, ys):
        copy_d2(dy).wait_recv()
        total = total + hr[lax.rem(y - dy + ys, ys)].astype(F32)
    mixed[...] = total

    sent = dot(dispatch, mixed[...].astype(BF16))
    sd[...] = sent.reshape(n, cap, share).astype(BF16)

    def copy_c1(d):
        peer = up(d)
        return remote(sd.at[peer], rows.at[t, e], sc1.at[d], rc1.at[d], {"ep": peer})

    def copy_c2(dy, d):
        src = down_of(d)
        to = lax.rem(y + dy, ys) * 2 + core
        return remote(rows.at[t, src], rows.at[t, src], sc2.at[dy, d], rc2.at[dy, d], {"tp": to})

    def copy_c3(dy, d):
        src = down_of(d)
        held = lax.rem(y - dy + ys, ys) * 2 + core
        return remote(rows.at[held, src], rows.at[held, src], sc3.at[dy, d], rc3.at[dy, d], {"tp": q})

    order = [dz * nx + dx for dz in far_first for dx in range(nx) if dz + dx]
    for d in order:
        copy_c1(d).start()

    rows[t, e] = sd[e]

    def spread(d):
        for dy in range(1, ys):
            copy_c2(dy, d).start()
        copy_c3(0, d).start()

    def relay(d):
        for dy in range(1, ys):
            copy_c2(dy, d).wait_recv()
            copy_c3(dy, d).start()

    near = order[::-1]
    spread(0)
    for i, d in enumerate(near):
        copy_c1(d).wait_recv()
        spread(d)
        if i >= 1:
            relay(([0] + near)[i - 1])
    for d in ([0] + near)[len(near) - 1:]:
        relay(d)
    for d in range(n):
        for dy in range(ys):
            copy_c3(dy, d).wait_recv()

    gs = min(n, max(1, 64 // cap))
    span = gs * cap

    @pl.loop(0, n // gs)
    def _(g):
        def piece(i):
            return rows[i, pl.ds(g * gs, gs)].astype(F32).reshape(span, share)

        acc = jnp.zeros((span, 1), F32)
        for i in range(p):
            v = piece(i)
            acc = acc + jnp.sum(v * v, axis=1, keepdims=True)
        sc = lax.rsqrt(acc / width + 1e-06)
        for i in range(p):
            cs = slice(i * share, (i + 1) * share)
            xn[pl.ds(pl.multiple_of(g * span, span), span), cs] = (
                piece(i) * sc * moe_gain[:, cs]
            ).astype(BF16)

    loads[5].wait()
    loads[6].wait()
    hidden = hid.shape[1]
    fc = min(256, hidden)

    @pl.loop(0, hidden // fc)
    def _(c):
        cs = pl.ds(pl.multiple_of(c * fc, fc), fc)
        gate_part = dot(xn[...], weg[:, cs])
        up_part = dot(xn[...], weu[:, cs])
        hid[:, cs] = (jax.nn.silu(gate_part) * up_part).astype(BF16)

    loads[7].wait()

    def copy_e1(yy):
        return remote(e_p.at[yy], e_r.at[yy], se1.at[yy], re1.at[yy], {"tp": q})

    def copy_e2(dy, dz):
        ty = lax.rem(y + dy, ys)
        zc = lax.rem(z + dz, nz)
        return remote(
            es.at[ty, zc], er.at[y, zc], se2.at[dy, dz], re2.at[dy, dz], {"tp": ty * 2 + core}
        )

    def copy_e3(d):
        peer = up(d)
        return remote(outb.at[peer], ret.at[e], se3.at[d], re3.at[d], {"ep": peer})

    nc = min(256, share)
    chunk = nx * cap

    def down(yy, parity, dst):
        @pl.loop(0, share // nc)
        def _(c):
            at = pl.ds(pl.multiple_of((yy * 2 + parity) * share + c * nc, nc), nc)
            value = dot(hid[...], wed[:, at]).reshape(nz, chunk, nc)
            dst[yy, :, :, pl.ds(pl.multiple_of(c * nc, nc), nc)] = value.astype(dst.dtype)

    for dy in list(range(1, ys)) + [0]:
        ty = lax.rem(y + dy, ys)
        down(ty, 1 - core, e_p)
        copy_e1(ty).start()
        down(ty, core, e_o)
        copy_e1(ty).wait_recv()
        if dy:
            for dz in far_first:
                zc = lax.rem(z + dz, nz)
                es[ty, zc] = (e_o[ty, zc] + e_r[ty, zc].astype(F32)).astype(BF16)
                copy_e2(dy, dz).start()
    for dz in far_first:
        zc = lax.rem(z + dz, nz)
        result = e_o[y, zc] + e_r[y, zc].astype(F32)
        for dy in range(1, ys):
            copy_e2(dy, dz).wait_recv()
            result = result + er[lax.rem(y - dy + ys, ys), zc].astype(F32)
        outb[pl.ds(zc * nx, nx)] = result.reshape(nx, cap, share).astype(BF16)
        for dx in range(nx):
            if dz + dx:
                copy_e3(dz * nx + dx).start()

    ret[e] = outb[e]
    for d in order:
        copy_e3(d).wait_recv()

    back = ret[...].astype(F32).reshape(slots, share).astype(BF16)

    def combine(weights):
        return lax.dot_general(weights, back, (((0,), (0,)), ((), ())), preferred_element_type=F32)

    layer_out[...] = (mixed[...] + combine(comb_hi) + combine(comb_lo)).astype(BF16)

    @pl.loop(1, n)
    def _(d):
        copy_a(d).wait_send()
        copy_a2(d).wait_send()
        copy_c1(d).wait_send()
        copy_e3(d).wait_send()

    @pl.loop(0, n)
    def _(d):
        for dy in range(1, ys):
            copy_c2(dy, d).wait_send()
        for dy in range(ys):
            copy_c3(dy, d).wait_send()

    for dy in range(ys):
        copy_d1(dy).wait_send()
        copy_e1(dy).wait_send()
    for dy in range(1, ys):
        copy_d2(dy).wait_send()
        for dz in range(nz):
            copy_e2(dy, dz).wait_send()
    for dz in range(nz):
        for dx in range(1, nx):
            copy_b(dz, dx).wait_send()
        if dz:
            copy_bz(dz).wait_send()


def finish(layer_in, state_in, moved, conv_in, layer_out, state_out, conv_out):
    layer_out[...] = layer_in[...]
    state_out[...] = state_in[...]
    kept = conv_in.shape[0] - 1
    for i in range(kept):
        conv_out[i] = conv_in[i + 1]
    conv_out[kept] = moved[...]


def shards(
    n, p,
    tokens, state_in, conv_in, mix_gain, rnn_weight, gate_weight, conv_weight, rate_weight,
    input_weight, rate_param, out_weight, moe_gain, expert_gate, expert_up, expert_down, routes, route_prob,
):
    g, width = tokens.shape
    depth, chans = rnn_weight.shape
    share = width // p
    cap = max(2, 2 * g * routes.shape[1] // n)
    slots = n * cap
    hidden = expert_gate.shape[2]
    ys = p // 2
    nx = 1 << ((n.bit_length() - 1) // 2)
    nx = nx if n % nx == 0 else 1
    nz = n // nx
    conv_t = jnp.transpose(conv_in, (1, 0, 2))
    vm = pl.BlockSpec(memory_space=pltpu.VMEM)
    hb = pl.BlockSpec(memory_space=pl.ANY)
    dma = pltpu.SemaphoreType.DMA
    V = pltpu.VMEM
    scratch = [
        V((depth, chans), BF16), V((depth, chans), BF16),
        V(rate_weight.shape, BF16), V(input_weight.shape, BF16), V(out_weight.shape, BF16),
        V(expert_gate.shape[1:], BF16), V(expert_up.shape[1:], BF16), V(expert_down.shape[1:], BF16),
        V((1, width), F32), V((1, width), F32),
        V((n, g, depth), BF16), V((n, g, depth), BF16),
        V((nz, nx, g, 2 * chans), BF16), V((nz, nx, g, 2 * chans), BF16),
        V((nz, g, 2 * chans), BF16), V((nz, g, 2 * chans), BF16),
        V((g, chans), BF16),
        V((ys, g, share), BF16), V((ys, g, share), F32), V((ys, g, share), BF16),
        V((ys, g, share), BF16), V((ys, g, share), BF16), V((g, share), F32),
        V((n, cap, share), BF16), V((p, n, cap, share), BF16), V((slots, width), BF16), V((slots, hidden), BF16),
        V((ys, nz, nx * cap, share), BF16), V((ys, nz, nx * cap, share), F32), V((ys, nz, nx * cap, share), BF16),
        V((ys, nz, nx * cap, share), BF16), V((ys, nz, nx * cap, share), BF16),
        V((n, cap, share), BF16), V((n, cap, share), BF16),
        dma((8,)),
        dma((n,)), dma((n,)), dma((n,)), dma((n,)), dma((nz, nx)), dma((nz, nx)), dma((nz,)), dma((nz,)),
        dma((ys,)), dma((ys,)), dma((ys,)), dma((ys,)),
        dma((n,)), dma((n,)), dma((ys, n)), dma((ys, n)), dma((ys, n)), dma((ys, n)),
        dma((ys,)), dma((ys,)), dma((ys, nz)), dma((ys, nz)), dma((n,)), dma((n,)),
    ]
    layer, state, moved = pl.pallas_call(
        functools.partial(kernel, n, p, nx, cap),
        out_shape=(
            jax.ShapeDtypeStruct((g, share), BF16),
            jax.ShapeDtypeStruct((g, chans), F32),
            jax.ShapeDtypeStruct((g, chans), BF16),
        ),
        in_specs=[vm] * 9 + [hb] * 8,
        out_specs=(vm, vm, vm),
        scratch_shapes=scratch,
        compiler_params=pltpu.CompilerParams(
            collective_id=0, has_side_effects=True, vmem_limit_bytes=60 * 1024 * 1024
        ),
    )(
        tokens, state_in, conv_t, mix_gain.reshape(-1, 128), moe_gain.reshape(-1, 128),
        conv_weight, rate_param[None], routes.T, route_prob.T,
        rnn_weight, gate_weight, rate_weight, input_weight, out_weight, expert_gate, expert_up, expert_down,
    )
    layer_out, state_out, conv_out = pl.pallas_call(
        finish,
        out_shape=(
            jax.ShapeDtypeStruct(layer.shape, layer.dtype),
            jax.ShapeDtypeStruct(state.shape, state.dtype),
            jax.ShapeDtypeStruct(conv_t.shape, conv_t.dtype),
        ),
        in_specs=[vm] * 4,
        out_specs=(vm, vm, vm),
    )(layer, state, moved, conv_t)
    return (layer_out, state_out, jnp.transpose(conv_out, (1, 0, 2)))


def solution(mesh):
    in_specs = (
        P("ep", None),
        P("ep", "tp"),
        P("ep", None, "tp"),
        P(),
        P("ep", "tp"),
        P("ep", "tp"),
        P(None, "tp"),
        P("tp", None, None),
        P("tp", None, None),
        P("tp"),
        P("tp", None),
        P(),
        P("ep", None, "tp"),
        P("ep", None, "tp"),
        P("ep", "tp", None),
        P("ep", None),
        P("ep", None),
    )
    out_specs = (P("ep", "tp"), P("ep", "tp"), P("ep", None, "tp"))
    body = functools.partial(shards, mesh.shape["ep"], mesh.shape["tp"])
    return jax.shard_map(body, mesh=mesh, in_specs=in_specs, out_specs=out_specs, check_vma=False)
```
